128 devices in a mesh: fs: 16 (over z, y), tp: 8 (over x, core).
Axes of the slice: x: 4, y: 4, z: 4, core: 2. Of those that a mesh axis runs over, the one named last changes fastest.
Arguments:
- saved_input: bfloat16 [196608, 2048], P(('fs', 'tp')), may hold values from -6 to 6
- key_cot: bfloat16 [196608, 1024], P(('fs', 'tp')), may hold values from -0.020184243 to 0.020184243
- mixed_out: bfloat16 [196608, 1024], P(('fs', 'tp')), may hold values from -6 to 6
- out_cot: bfloat16 [196608, 2048], P(('fs', 'tp')), may hold values from -0.020184243 to 0.020184243
- key_weight: float32 [2048, 1024], P('fs', 'tp'), may hold values from -0.125 to 0.125
- out_weight: float32 [1024, 2048], P('tp', 'fs'), may hold values from -0.1875 to 0.1875
- bases: bfloat16 [2, 1024, 512], replicated, may hold values from -0.1875 to 0.1875
- first_moment: float32 [2, 2048, 512], P(None, 'fs', 'tp'), may hold values from -64 to 64
- second_moment: float32 [2, 2048, 512], P(None, 'fs', 'tp'), may hold values from 0.25 to 4
Outputs:
- key_weight_new: float32 [2048, 1024], P('fs', 'tp')
- out_weight_new: float32 [1024, 2048], P('tp', 'fs')
- key_step: float32 [2048, 1024], P('fs', 'tp')
- out_step: float32 [1024, 2048], P('tp', 'fs')
- first_new: float32 [2, 2048, 512], P(None, 'fs', 'tp')
- second_new: float32 [2, 2048, 512], P(None, 'fs', 'tp')
- key_copy: bfloat16 [2048, 1024], P(None, 'tp')
- out_copy: bfloat16 [1024, 2048], P('tp')
The draws below stay inside these ranges and needn't reach their ends.
All inputs are finite; a program needn't handle non-finite values.
Results may differ from the reference program's by a relative error of at most 0.0032.
Values may be sent and summed in bfloat16 or wider, within the bound.
No kernel may reach another device: no remote copies, remote signals or barrier semaphores. Data moves between devices by JAX's collectives and lax.ppermute only.
A program may use at most 128 MiB of HBM per device.

```python
import math
import jax
import jax.numpy as jnp
from jax import lax

D = 2048
KEY_WIDTH = 1024
RANK = 512
TOK_DEV = 1536
TOKENS = 196608


def scaled_moment(key, rows, cols):
    row_key, col_key, base_key = jax.random.split(key, 3)
    low_end, high_end = (0.3, 3.0)
    row_scale = jnp.exp(jax.random.uniform(row_key, (2, rows, 1), jnp.float32, math.log(low_end), math.log(high_end)))
    col_scale = jnp.exp(jax.random.uniform(col_key, (2, 1, cols), jnp.float32, math.log(low_end), math.log(high_end)))
    normals = jnp.clip(jax.random.normal(base_key, (2, rows, cols), jnp.float32), -4.0, 4.0)
    return normals * row_scale * col_scale


def draw_first_moment(key, part):
    return scaled_moment(jax.random.fold_in(key, 11), D, RANK)


def input_like(key, row_tag, col_tag, width):
    noise = jax.random.normal(jax.random.fold_in(key, col_tag + 1000), (TOKENS, width), jnp.float32)
    return jnp.clip(noise, -6.0, 6.0)


def cotangent_like(key, row_tag, col_tag, width):
    noise = jax.random.normal(jax.random.fold_in(key, col_tag + 1000), (TOKENS, width), jnp.float32)
    spread = float(TOKENS) ** (-0.5)
    column_scale = jnp.exp(jax.random.uniform(jax.random.fold_in(key, col_tag + 2000), (1, width), jnp.float32, math.log(0.5), math.log(2.0)))
    return spread * jnp.clip(noise, -4.0, 4.0) * column_scale


def draw_saved_input(key, part):
    return input_like(key, 101, 201, D).astype(jnp.bfloat16)


def draw_key_cot(key, part):
    return cotangent_like(key, 101, 202, KEY_WIDTH).astype(jnp.bfloat16)


def draw_mixed_out(key, part):
    return input_like(key, 102, 203, KEY_WIDTH).astype(jnp.bfloat16)


def draw_out_cot(key, part):
    return cotangent_like(key, 102, 204, D).astype(jnp.bfloat16)


def levels(key, extent, cuts, smallest, largest):
    loudness = 1.0
    for axis_at, blocks in cuts:
        draws = jax.random.uniform(jax.random.fold_in(jax.random.fold_in(key, 6), axis_at), (blocks,), jnp.float32, smallest / len(cuts), largest / len(cuts))
        loudness = loudness * jnp.repeat(jnp.exp(draws), extent[axis_at] // blocks).reshape((-1,) + (1,) * (len(extent) - 1 - axis_at))
    return loudness


def bell_draw(rng, shape, scale, reach, cuts=(), dtype=jnp.bfloat16):
    drawn = jax.random.normal(rng, shape, jnp.float32) * scale
    if len(cuts) > 0:
        drawn = levels(rng, shape, cuts, -0.22, 0.18) * drawn
    return jnp.clip(drawn, min=-reach, max=reach).astype(dtype)


def setup_inputs(seed: int = 0) -> dict:
    key_of = jax.random.split(jax.random.key(seed), 10)
    saved_input = draw_saved_input(jax.random.fold_in(key_of[9], 71), 0)
    key_cot = draw_key_cot(jax.random.fold_in(key_of[9], 71), 0)
    mixed_out = draw_mixed_out(jax.random.fold_in(key_of[9], 71), 0)
    out_cot = draw_out_cot(jax.random.fold_in(key_of[9], 71), 0)
    key_weight = bell_draw(key_of[4], (D, KEY_WIDTH), D ** -0.5, 0.125, ((0, 16), (1, 8)), jnp.float32)
    out_weight = bell_draw(key_of[5], (KEY_WIDTH, D), KEY_WIDTH ** -0.5, 0.1875, ((0, 8), (1, 16)), jnp.float32)
    bases = bell_draw(key_of[6], (2, KEY_WIDTH, RANK), KEY_WIDTH ** -0.5, 0.1875)
    first_moment = draw_first_moment(jax.random.fold_in(key_of[9], 71), 0)
    second_moment = jnp.clip(jnp.exp(math.log(4.0) - 2.7725887 * jax.random.uniform(key_of[8], (2, D, RANK), jnp.float32) ** levels(key_of[8], (2, D, RANK), ((1, 16), (2, 8)), -0.2, 0.2)), 0.25, 4.0)
    return {"saved_input": saved_input, "key_cot": key_cot, "mixed_out": mixed_out, "out_cot": out_cot, "key_weight": key_weight, "out_weight": out_weight, "bases": bases, "first_moment": first_moment, "second_moment": second_moment}


highest = lax.Precision.HIGHEST
first_decay = 0.8
second_decay = 0.9
learn_rate = 0.01

def reference(saved_input, key_cot, mixed_out, out_cot, key_weight, out_weight, bases, first_moment, second_moment):
    blocks = saved_input.shape[0] // TOK_DEV

    def in_blocks(array):
        return array.reshape(blocks, TOK_DEV, array.shape[1])

    def accumulate(running, pieces):
        inputs_part, key_part, mixed_part, cot_part = pieces
        key_grad = jnp.dot(inputs_part.astype(jnp.float32).T, key_part.astype(jnp.float32), precision=highest)
        out_grad_t = jnp.dot(cot_part.astype(jnp.float32).T, mixed_part.astype(jnp.float32), precision=highest)
        return ((running[0] + key_grad, running[1] + out_grad_t), None)
    empty_sum = jnp.zeros((D, KEY_WIDTH), jnp.float32)
    totals, _ = lax.scan(accumulate, (empty_sum, empty_sum), (in_blocks(saved_input), in_blocks(key_cot), in_blocks(mixed_out), in_blocks(out_cot)))
    gradients = jnp.stack(totals)
    bases_wide = bases.astype(jnp.float32)
    reduced = jnp.einsum('mrk,mkq->mrq', gradients, bases_wide, precision=highest)
    first_new = first_decay * first_moment + (1.0 - first_decay) * reduced
    second_new = second_decay * second_moment + (1.0 - second_decay) * reduced * reduced
    direction = first_new / jnp.sqrt(second_new)
    scales = lax.rsqrt(lax.optimization_barrier(jnp.mean(direction * direction, axis=(1, 2))) + 1.0)
    projected = jnp.einsum('mrq,mkq->mrk', direction, bases_wide, precision=highest)
    scaled = projected * scales[:, None, None]
    key_step = scaled[0]
    out_step = scaled[1].T
    key_new = key_weight - learn_rate * key_step
    out_new = out_weight - learn_rate * out_step
    return (key_new, out_new, key_step, out_step, first_new, second_new, key_new.astype(jnp.bfloat16), out_new.astype(jnp.bfloat16))
```

```python
import jax
import jax.numpy as jnp
from jax import lax
from jax.sharding import Mesh
from jax.sharding import PartitionSpec as P

D = 2048
RANK = 512
TP = ("tp_0", "tp_1")
FS = ("fs_0", "fs_1")
CHIPS = ("fs_0", "fs_1", "tp_0")
FS_TP = ("fs_0", "fs_1", "tp_0", "tp_1")
SWAP = [(0, 1), (1, 0)]


highest = lax.Precision.HIGHEST
first_decay = 0.8
second_decay = 0.9
learn_rate = 0.01


def exchanged(tiles, axes):
    return lax.all_to_all(tiles, axes, split_axis=0, concat_axis=0, tiled=True)


def swapped(array):
    return lax.ppermute(array, "tp_1", SWAP)


def pick(core, zero, one):
    return jnp.where(core == 0, zero, one)


def low_rank(rows, cols, base):
    mapped = jnp.dot(cols, base, preferred_element_type=jnp.float32).astype(jnp.bfloat16)
    return lax.dot_general(
        mapped, rows, (((0,), (0,)), ((), ())), preferred_element_type=jnp.float32
    )


def body(
    saved_input,
    key_cot,
    mixed_out,
    out_cot,
    key_weight,
    out_weight,
    bases,
    first_moment,
    second_moment,
):
    core = lax.axis_index("tp_1")
    chip_x = lax.axis_index("tp_0")
    n_fs = lax.axis_size(FS)
    n_x = lax.axis_size("tp_0")
    rows = key_weight.shape[0]
    cols = key_weight.shape[1]
    half = first_moment.shape[2]
    width = 2 * half

    def key_low():
        return low_rank(saved_input, key_cot, bases[0])

    def out_low():
        return low_rank(out_cot, mixed_out, bases[1])

    theirs = lax.cond(
        core == 0, lambda: out_low().astype(jnp.bfloat16), lambda: key_low().astype(jnp.bfloat16)
    )
    from_partner = swapped(theirs)
    mine = lax.cond(core == 0, key_low, out_low)
    chip_sum = (mine + from_partner.astype(jnp.float32)).astype(jnp.bfloat16)
    tiles = chip_sum.reshape(n_x, width, n_fs, rows).transpose(2, 0, 1, 3)
    arrived = exchanged(tiles.reshape(n_fs * n_x, width, rows), CHIPS)
    low = arrived.astype(jnp.float32).sum(axis=0)

    moments = jnp.stack((first_moment, second_moment), axis=1).transpose(0, 1, 3, 2)
    kept = pick(core, moments[0], moments[1])
    got = swapped(pick(core, moments[1], moments[0]))
    both = jnp.concatenate((pick(core, kept, got), pick(core, got, kept)), axis=1)
    first = first_decay * both[0] + (1.0 - first_decay) * low
    second = second_decay * both[1] + (1.0 - second_decay) * low * low
    direction = first / jnp.sqrt(second)

    square = jnp.sum(direction * direction)
    lanes = lax.broadcasted_iota(jnp.int32, (1, 128), 1)
    row = jnp.where(lanes == core, square, 0.0)
    everyone = lax.axis_size(FS_TP)
    sums = exchanged(jnp.broadcast_to(row[None], (everyone, 1, 128)), FS_TP).sum(axis=0)
    scales = lax.rsqrt(sums[0] / (D * RANK) + 1.0)

    shifted = [direction] + [
        lax.ppermute(direction, "tp_0", [(i, (i + s) % n_x) for i in range(n_x)])
        for s in range(1, n_x)
    ]
    base = pick(core, bases[0], bases[1])
    base = lax.dynamic_slice_in_dim(base, chip_x * 2 * cols, 2 * cols, 0).astype(jnp.float32)
    projected = 0.0
    for s in range(n_x):
        block = lax.dynamic_slice_in_dim(base, (chip_x - s) % n_x * width, width, 1)
        projected = projected + jnp.dot(
            block, shifted[s], precision=highest, preferred_element_type=jnp.float32
        )
    left, right = (projected[:cols], projected[cols:])
    own = pick(core, left, right)
    other = swapped(pick(core, right, left))
    key_step = pick(core, own, other).T * scales[0]
    out_step = pick(core, other, own) * scales[1]
    key_new = key_weight - learn_rate * key_step
    out_new = out_weight - learn_rate * out_step
    copies = jnp.stack((key_new.astype(jnp.bfloat16), out_new.astype(jnp.bfloat16)))
    gathered = exchanged(jnp.broadcast_to(copies[None], (n_fs, *copies.shape)), FS)
    key_copy = gathered[:, 0].reshape(n_fs * rows, cols)
    out_copy = gathered[:, 1].transpose(1, 0, 2).reshape(cols, n_fs * rows)

    news = jnp.stack((first, second))
    low_half, high_half = (news[:, :half], news[:, half:])
    stay = pick(core, low_half, high_half)
    come = swapped(pick(core, high_half, low_half))
    key_moments = pick(core, stay, come)
    out_moments = pick(core, come, stay)
    first_new = jnp.stack((key_moments[0], out_moments[0])).transpose(0, 2, 1)
    second_new = jnp.stack((key_moments[1], out_moments[1])).transpose(0, 2, 1)
    return (key_new, out_new, key_step, out_step, first_new, second_new, key_copy, out_copy)


def solution(mesh):
    torus = Mesh(mesh.devices.reshape(4, 4, 4, 2), ("fs_0", "fs_1", "tp_0", "tp_1"))
    placed = (
        P(FS_TP, None),
        P(FS_TP, None),
        P(FS_TP, None),
        P(FS_TP, None),
        P(FS, TP),
        P(TP, FS),
        P(),
        P(None, FS, TP),
        P(None, FS, TP),
    )
    return jax.shard_map(
        body,
        mesh=torus,
        in_specs=placed,
        out_specs=(
            P(FS, TP),
            P(TP, FS),
            P(FS, TP),
            P(TP, FS),
            P(None, FS, TP),
            P(None, FS, TP),
            P(None, TP),
            P(TP, None),
        ),
        check_vma=False,
    )
```

```python
import functools

import jax
import jax.numpy as jnp
from jax import lax
from jax.experimental import pallas as pl
from jax.experimental.pallas import tpu as pltpu
from jax.sharding import Mesh
from jax.sharding import PartitionSpec as P

D = 2048
RANK = 512
FS = ("fs_0", "fs_1")
TP = ("tp_0", "tp_1")
CHIPS = ("fs_0", "tp_0", "fs_1")
ROWS_AND_CORE = ("tp_1", "fs_0", "fs_1")
FS_TP = ("fs_0", "fs_1", "tp_0", "tp_1")
SWAP = [(0, 1), (1, 0)]
LANES = 128
MIB = 2**20


first_decay = 0.8
second_decay = 0.9
learn_rate = 0.01

wide = jnp.float32
narrow = jnp.bfloat16
in_smem = pl.BlockSpec(memory_space=pltpu.SMEM)
in_hbm = pl.BlockSpec(memory_space=pltpu.HBM)
in_vmem = pl.BlockSpec(memory_space=pltpu.VMEM)


def exchanged(tiles, axes):
    return lax.all_to_all(tiles, axes, split_axis=0, concat_axis=0, tiled=True)


def swapped(array):
    return lax.ppermute(array, "tp_1", SWAP)


def pick(core, zero, one):
    return jnp.where(core == 0, zero, one)


PARTS = 3
CHUNKS = 8


def map_part(i, cols, base, mapped):
    part = cols.shape[0] // PARTS
    at = pl.ds(i * part, part)
    block = jnp.dot(cols[at, :], base[...], preferred_element_type=wide)
    mapped[:, at] = block.astype(narrow).T


def contract(mapped, rows, out):
    chunk = out.shape[1] // CHUNKS
    for j in range(CHUNKS):
        at = pl.ds(j * chunk, chunk)
        total, start = (None, 0)
        for piece in rows:
            length = piece.shape[0]
            block = jnp.dot(
                mapped[:, start : start + length], piece[:, at], preferred_element_type=wide
            )
            total = block if total is None else total + block
            start += length
        out[:, at] = total.astype(out.dtype)


def partner_kernel(
    core, rows0, cols0, rows1, cols1, bases, out, rows2, cols2, base2, rows, cols, base, mapped, sems
):
    part = cols.shape[0] // PARTS
    early = rows2.shape[0]

    def base_load(k):
        matrix = core[0] if k else 1 - core[0]
        return pltpu.make_async_copy(bases.at[matrix], (base, base2)[k], sems.at[k])

    def cols_load(source, i):
        at = pl.ds(i * part, part)
        return pltpu.make_async_copy(source.at[at], cols.at[at], sems.at[2 + i])

    def rows_load(source):
        return pltpu.make_async_copy(source, rows, sems.at[5])

    def own_cols_load(source):
        return pltpu.make_async_copy(source, cols2, sems.at[6])

    def own_rows_load(source):
        return pltpu.make_async_copy(source.at[pl.ds(0, early)], rows2, sems.at[7])

    def start(zero, load, first, second):
        @pl.when(core[0] == zero)
        def _():
            load(first).start()

        @pl.when(core[0] != zero)
        def _():
            load(second).start()

    base_load(0).start()
    for i in range(PARTS):
        start(1, lambda source, i=i: cols_load(source, i), cols0, cols1)
    base_load(0).wait()
    for i in range(PARTS):
        cols_load(cols0, i).wait()
        if i == 0:
            start(1, rows_load, rows0, rows1)
        map_part(i, cols, base, mapped)
    rows_load(rows0).wait()
    base_load(1).start()
    start(0, own_cols_load, cols0, cols1)
    start(0, own_rows_load, rows0, rows1)
    contract(mapped, (rows,), out)
    base_load(1).wait()
    own_cols_load(cols0).wait()
    own_rows_load(rows0).wait()


def own_kernel(core, rows0, rows1, rows, cols, base, out, late, mapped, sem):
    def late_load(source):
        return pltpu.make_async_copy(source.at[pl.ds(rows.shape[0], late.shape[0])], late, sem)

    @pl.when(core[0] == 0)
    def _():
        late_load(rows0).start()

    @pl.when(core[0] != 0)
    def _():
        late_load(rows1).start()

    for i in range(PARTS):
        map_part(i, cols, base, mapped)
    late_load(rows0).wait()
    contract(mapped, (rows, late), out)


def cost_of(tokens, height, width, rank):
    return pl.CostEstimate(
        flops=2 * tokens * rank * (height + width),
        bytes_accessed=2 * tokens * (height + width),
        transcendentals=0,
    )


def both_low(core, saved_input, key_cot, out_cot, mixed_out, bases):
    tokens, height = saved_input.shape
    _, width, rank = bases.shape
    early = tokens // 2
    cost = cost_of(tokens, height, width, rank)
    rows0, cols0, rows1, cols1, in_bases = (
        pltpu.with_memory_space_constraint(a, pltpu.HBM)
        for a in (saved_input, key_cot, out_cot, mixed_out, bases)
    )
    theirs, rows, cols, base = pl.pallas_call(
        partner_kernel,
        out_shape=(
            pltpu.VMEM((rank, height), narrow),
            pltpu.VMEM((early, height), narrow),
            pltpu.VMEM((tokens, width), narrow),
            pltpu.VMEM((width, rank), narrow),
        ),
        in_specs=[in_smem] + [in_hbm] * 5,
        out_specs=(in_vmem,) * 4,
        scratch_shapes=[
            pltpu.VMEM((tokens, height), narrow),
            pltpu.VMEM((tokens, width), narrow),
            pltpu.VMEM((width, rank), narrow),
            pltpu.VMEM((rank, tokens), narrow),
            pltpu.SemaphoreType.DMA((8,)),
        ],
        compiler_params=pltpu.CompilerParams(vmem_limit_bytes=20 * MIB),
        cost_estimate=cost,
        name="partner_low",
    )(core, rows0, cols0, rows1, cols1, in_bases)
    from_partner = swapped(theirs)
    mine = pl.pallas_call(
        own_kernel,
        out_shape=pltpu.VMEM((rank, height), wide),
        in_specs=[in_smem] + [in_hbm] * 2 + [in_vmem] * 3,
        out_specs=in_vmem,
        scratch_shapes=[
            pltpu.VMEM((tokens - early, height), narrow),
            pltpu.VMEM((rank, tokens), narrow),
            pltpu.SemaphoreType.DMA,
        ],
        compiler_params=pltpu.CompilerParams(vmem_limit_bytes=14 * MIB),
        cost_estimate=cost,
        name="own_low",
    )(core, rows0, rows1, rows, cols, base)
    return mine, from_partner


def combine_kernel(mine, partner, out, tiles, sems, *, n_x, n_y):
    count = out.shape[0] // sems.shape[0]
    for z in range(sems.shape[0]):
        for x in range(n_x):
            for y in range(n_y):
                ranks, rows = (pl.ds(x * LANES, LANES), pl.ds((z * n_y + y) * LANES, LANES))
                total = mine[ranks, rows] + partner[ranks, rows].astype(wide)
                tiles[(z * n_x + x) * n_y + y] = total.astype(narrow)
        at = pl.ds(z * count, count)
        pltpu.make_async_copy(tiles.at[at], out.at[at], sems.at[z]).start()
    for z in range(sems.shape[0]):
        at = pl.ds(z * count, count)
        pltpu.make_async_copy(tiles.at[at], out.at[at], sems.at[z]).wait()


def combine(mine, partner, n_z, n_y, n_x):
    shape = (n_z * n_y * n_x, LANES, LANES)
    return pl.pallas_call(
        functools.partial(combine_kernel, n_x=n_x, n_y=n_y),
        out_shape=pltpu.HBM(shape, narrow),
        in_specs=[in_vmem] * 2,
        out_specs=in_hbm,
        scratch_shapes=[pltpu.VMEM(shape, narrow), pltpu.SemaphoreType.DMA((n_z,))],
        compiler_params=pltpu.CompilerParams(vmem_limit_bytes=8 * MIB),
        name="combine",
    )(mine, partner)


def moments_kernel(core, low, firsts, seconds, got, first, second, direction):
    zero = core[0] == 0

    def joined(old, came):
        kept = jnp.where(zero, old[0], old[1])
        return jnp.concatenate((jnp.where(zero, kept, came), jnp.where(zero, came, kept)), axis=0)

    sums = low[...]
    first_new = first_decay * joined(firsts, got[0]) + (1.0 - first_decay) * sums
    second_new = second_decay * joined(seconds, got[1]) + (1.0 - second_decay) * sums * sums
    first[...] = first_new
    second[...] = second_new
    direction[...] = first_new / jnp.sqrt(second_new)


def new_moments(core, low, firsts, seconds, got):
    return pl.pallas_call(
        moments_kernel,
        out_shape=(pltpu.VMEM(low.shape, wide),) * 3,
        in_specs=[in_smem] + [in_vmem] * 4,
        out_specs=(in_vmem,) * 3,
        compiler_params=pltpu.CompilerParams(vmem_limit_bytes=4 * MIB),
        name="moments",
    )(core, low, firsts, seconds, got)


def project_kernel(where, bases, *refs):
    *directions, own, other, row, base, sem = refs
    core, chip_x = (where[0], where[1])
    cols = own.shape[0]
    n_x = len(directions)
    at = pl.ds(pl.multiple_of(chip_x * 2 * cols, 2 * cols), 2 * cols)
    load = pltpu.make_async_copy(bases.at[core, at], base, sem)
    load.start()
    square = jnp.zeros((1, LANES), wide)
    parts = []
    for x in range(n_x):
        part = directions[0][...]
        back = lax.rem(chip_x - x + n_x, n_x)
        for s in range(1, n_x):
            part = jnp.where(back == s, directions[s][...], part)
        square = square + jnp.sum(part * part, axis=0, keepdims=True)
        parts.append(part)
    square = jnp.sum(square, axis=1, keepdims=True)
    lanes = lax.broadcasted_iota(jnp.int32, (1, LANES), 1)
    row[...] = jnp.broadcast_to(jnp.where(lanes == core, square, 0.0)[None], row.shape)
    load.wait()
    total = jnp.zeros((2 * cols, parts[0].shape[1]), wide)
    for x, part in enumerate(parts):
        width, n = part.shape
        high = part.astype(narrow)
        rest = part - high.astype(wide)
        middle = rest.astype(narrow)
        low = (rest - middle.astype(wide)).astype(narrow)
        limbs = jnp.concatenate((high, middle, low), axis=1)
        product = jnp.dot(
            base[:, x * width : (x + 1) * width], limbs, preferred_element_type=wide
        )
        total = total + (product[:, :n] + (product[:, n : 2 * n] + product[:, 2 * n :]))
    left, right = (total[:cols], total[cols:])
    own[...] = jnp.where(core == 0, left, right)
    other[...] = jnp.where(core == 0, right, left)


def project(where, bases, directions, cols, peers):
    out = pltpu.VMEM((cols, directions[0].shape[1]), wide)
    return pl.pallas_call(
        project_kernel,
        out_shape=(out, out, jax.ShapeDtypeStruct((peers, 1, LANES), wide)),
        in_specs=[in_smem, in_hbm] + [in_vmem] * len(directions),
        out_specs=(in_vmem,) * 3,
        scratch_shapes=[
            pltpu.VMEM((2 * cols, bases.shape[2]), narrow),
            pltpu.SemaphoreType.DMA,
        ],
        compiler_params=pltpu.CompilerParams(vmem_limit_bytes=6 * MIB),
        name="project",
    )(where, bases, *directions)


def steps_of(core, sums, own, came, key_weight, out_weight):
    total = jnp.sum(sums[...], axis=0)
    scales = lax.rsqrt(total / (D * RANK) + 1.0)
    lanes = lax.broadcasted_iota(jnp.int32, scales.shape, 1)
    key_scale = jnp.sum(jnp.where(lanes == 0, scales, 0.0), axis=1, keepdims=True)
    out_scale = jnp.sum(jnp.where(lanes == 1, scales, 0.0), axis=1, keepdims=True)
    zero = core[0] == 0
    key_step = jnp.where(zero, own[...], came[...]).T * key_scale
    out_step = jnp.where(zero, came[...], own[...]) * out_scale
    key_new = key_weight[...] - learn_rate * key_step
    out_new = out_weight[...] - learn_rate * out_step
    return (key_new, out_new, key_step, out_step)


def copies_kernel(core, sums, own, came, key_weight, out_weight, copies):
    key_new, out_new, _, _ = steps_of(core, sums, own, came, key_weight, out_weight)
    copies[...] = jnp.broadcast_to(
        jnp.stack((key_new.astype(narrow), out_new.astype(narrow)))[None], copies.shape
    )


def steps_kernel(core, sums, own, came, key_weight, out_weight, *outs):
    for out, value in zip(outs, steps_of(core, sums, own, came, key_weight, out_weight)):
        out[...] = value


def stepped(kernel, outs, *args):
    return pl.pallas_call(
        kernel,
        out_shape=outs,
        in_specs=[in_smem] + [in_vmem] * 5,
        out_specs=jax.tree.map(lambda _: in_vmem, outs),
        compiler_params=pltpu.CompilerParams(vmem_limit_bytes=6 * MIB),
    )(*args)


def spread_kernel(gathered, key_copy, out_copy, *, n_y):
    n_z = gathered.shape[0] // n_y
    for y in range(n_y):
        for z in range(n_z):
            at = pl.ds((z * n_y + y) * LANES, LANES)
            key_copy[at, :] = gathered[y * n_z + z, 0]
            out_copy[:, at] = gathered[y * n_z + z, 1]


def spread(gathered, n_y):
    n_fs, _, rows, cols = gathered.shape
    return pl.pallas_call(
        functools.partial(spread_kernel, n_y=n_y),
        out_shape=(
            jax.ShapeDtypeStruct((n_fs * rows, cols), narrow),
            jax.ShapeDtypeStruct((cols, n_fs * rows), narrow),
        ),
        in_specs=[in_vmem],
        out_specs=(in_vmem, in_vmem),
        compiler_params=pltpu.CompilerParams(vmem_limit_bytes=6 * MIB),
        name="spread",
    )(gathered)


def body(
    saved_input,
    key_cot,
    mixed_out,
    out_cot,
    key_weight,
    out_weight,
    bases,
    first_moment,
    second_moment,
):
    core = lax.axis_index("tp_1").astype(jnp.int32)
    chip_x = lax.axis_index("tp_0").astype(jnp.int32)
    n_z, n_y, n_x = (lax.axis_size(axis) for axis in ("fs_0", "fs_1", "tp_0"))
    rows, cols = key_weight.shape
    half = first_moment.shape[2]
    this = core.reshape(1)

    mine, from_partner = both_low(this, saved_input, key_cot, out_cot, mixed_out, bases)
    arrived = exchanged(combine(mine, from_partner, n_z, n_y, n_x), CHIPS)
    low = arrived.astype(wide).sum(axis=0)

    firsts = first_moment.transpose(0, 2, 1)
    seconds = second_moment.transpose(0, 2, 1)
    got = swapped(
        jnp.stack((pick(core, firsts[1], firsts[0]), pick(core, seconds[1], seconds[0])))
    )
    first, second, direction = new_moments(this, low, firsts, seconds, got)

    directions = [direction] + [
        lax.ppermute(direction, "tp_0", [(i, (i + s) % n_x) for i in range(n_x)])
        for s in range(1, n_x)
    ]
    own, other, row = project(
        jnp.stack((core, chip_x)), bases, directions, cols, lax.axis_size(ROWS_AND_CORE)
    )
    sums = exchanged(row, ROWS_AND_CORE)
    came = swapped(other)
    square = jax.ShapeDtypeStruct((rows, cols), wide)
    args = (this, sums, own, came, key_weight, out_weight)
    copies = stepped(copies_kernel, pltpu.HBM((n_z * n_y, 2, rows, cols), narrow), *args)
    gathered = exchanged(copies, ("fs_1", "fs_0"))
    key_new, out_new, key_step, out_step = stepped(steps_kernel, (square,) * 4, *args)
    key_copy, out_copy = spread(gathered, n_y)

    news = jnp.stack((first, second))
    low_half, high_half = (news[:, :half], news[:, half:])
    stay = pick(core, low_half, high_half)
    come = swapped(pick(core, high_half, low_half))
    key_moments = pick(core, stay, come)
    out_moments = pick(core, come, stay)
    first_new = jnp.stack((key_moments[0], out_moments[0])).transpose(0, 2, 1)
    second_new = jnp.stack((key_moments[1], out_moments[1])).transpose(0, 2, 1)
    return (key_new, out_new, key_step, out_step, first_new, second_new, key_copy, out_copy)


def solution(mesh):
    torus = Mesh(mesh.devices.reshape(4, 4, 4, 2), ("fs_0", "fs_1", "tp_0", "tp_1"))
    placed = (
        P(FS_TP, None),
        P(FS_TP, None),
        P(FS_TP, None),
        P(FS_TP, None),
        P(FS, TP),
        P(TP, FS),
        P(),
        P(None, FS, TP),
        P(None, FS, TP),
    )
    return jax.shard_map(
        body,
        mesh=torus,
        in_specs=placed,
        out_specs=(
            P(FS, TP),
            P(TP, FS),
            P(FS, TP),
            P(TP, FS),
            P(None, FS, TP),
            P(None, FS, TP),
            P(None, TP),
            P(TP, None),
        ),
        check_vma=False,
    )
```

```python
import functools

import jax
import jax.numpy as jnp
from jax import lax
from jax.experimental import pallas as pl
from jax.experimental.pallas import tpu as pltpu
from jax.sharding import Mesh
from jax.sharding import PartitionSpec as P

D = 2048
RANK = 512
FS = ("fs_0", "fs_1")
TP = ("tp_0", "tp_1")
CHIPS = ("fs_0", "tp_0", "fs_1")
FS_TP = ("fs_0", "fs_1", "tp_0", "tp_1")
SWAP = [(0, 1), (1, 0)]
LANES = 128
MIB = 2**20


first_decay = 0.8
second_decay = 0.9
learn_rate = 0.01

wide = jnp.float32
narrow = jnp.bfloat16
in_smem = pl.BlockSpec(memory_space=pltpu.SMEM)
in_hbm = pl.BlockSpec(memory_space=pltpu.HBM)
in_vmem = pl.BlockSpec(memory_space=pltpu.VMEM)


def exchanged(tiles, axes):
    return lax.all_to_all(tiles, axes, split_axis=0, concat_axis=0, tiled=True)


def swapped(array):
    return lax.ppermute(array, "tp_1", SWAP)


def pick(core, zero, one):
    return jnp.where(core == 0, zero, one)


PARTS = 3
CHUNKS = 8


def map_part(i, cols, base, mapped):
    part = cols.shape[0] // PARTS
    at = pl.ds(i * part, part)
    block = jnp.dot(cols[at, :], base[...], preferred_element_type=wide)
    mapped[:, at] = block.astype(narrow).T


def contract(mapped, rows, out):
    chunk = out.shape[1] // CHUNKS
    for j in range(CHUNKS):
        at = pl.ds(j * chunk, chunk)
        total, start = (None, 0)
        for piece in rows:
            length = piece.shape[0]
            block = jnp.dot(
                mapped[:, start : start + length], piece[:, at], preferred_element_type=wide
            )
            total = block if total is None else total + block
            start += length
        out[:, at] = total.astype(out.dtype)


def partner_kernel(
    core, rows0, cols0, rows1, cols1, bases, out, rows2, cols2, base2, rows, cols, base, mapped, sems
):
    part = cols.shape[0] // PARTS
    early = rows2.shape[0]

    def base_load(k):
        matrix = core[0] if k else 1 - core[0]
        return pltpu.make_async_copy(bases.at[matrix], (base, base2)[k], sems.at[k])

    def cols_load(source, i):
        at = pl.ds(i * part, part)
        return pltpu.make_async_copy(source.at[at], cols.at[at], sems.at[2 + i])

    def rows_load(source):
        return pltpu.make_async_copy(source, rows, sems.at[5])

    def own_cols_load(source):
        return pltpu.make_async_copy(source, cols2, sems.at[6])

    def own_rows_load(source):
        return pltpu.make_async_copy(source.at[pl.ds(0, early)], rows2, sems.at[7])

    def start(zero, load, first, second):
        @pl.when(core[0] == zero)
        def _():
            load(first).start()

        @pl.when(core[0] != zero)
        def _():
            load(second).start()

    base_load(0).start()
    for i in range(PARTS):
        start(1, lambda source, i=i: cols_load(source, i), cols0, cols1)
    base_load(0).wait()
    for i in range(PARTS):
        cols_load(cols0, i).wait()
        if i == 0:
            start(1, rows_load, rows0, rows1)
        map_part(i, cols, base, mapped)
    rows_load(rows0).wait()
    base_load(1).start()
    start(0, own_cols_load, cols0, cols1)
    start(0, own_rows_load, rows0, rows1)
    contract(mapped, (rows,), out)
    base_load(1).wait()
    own_cols_load(cols0).wait()
    own_rows_load(rows0).wait()


def own_kernel(core, rows0, rows1, rows, cols, base, out, late, mapped, sem):
    def late_load(source):
        return pltpu.make_async_copy(source.at[pl.ds(rows.shape[0], late.shape[0])], late, sem)

    @pl.when(core[0] == 0)
    def _():
        late_load(rows0).start()

    @pl.when(core[0] != 0)
    def _():
        late_load(rows1).start()

    for i in range(PARTS):
        map_part(i, cols, base, mapped)
    late_load(rows0).wait()
    contract(mapped, (rows, late), out)


def cost_of(tokens, height, width, rank):
    return pl.CostEstimate(
        flops=2 * tokens * rank * (height + width),
        bytes_accessed=2 * tokens * (height + width),
        transcendentals=0,
    )


def both_low(core, saved_input, key_cot, out_cot, mixed_out, bases):
    tokens, height = saved_input.shape
    _, width, rank = bases.shape
    early = tokens // 2
    cost = cost_of(tokens, height, width, rank)
    rows0, cols0, rows1, cols1, in_bases = (
        pltpu.with_memory_space_constraint(a, pltpu.HBM)
        for a in (saved_input, key_cot, out_cot, mixed_out, bases)
    )
    theirs, rows, cols, base = pl.pallas_call(
        partner_kernel,
        out_shape=(
            pltpu.VMEM((rank, height), narrow),
            pltpu.VMEM((early, height), narrow),
            pltpu.VMEM((tokens, width), narrow),
            pltpu.VMEM((width, rank), narrow),
        ),
        in_specs=[in_smem] + [in_hbm] * 5,
        out_specs=(in_vmem,) * 4,
        scratch_shapes=[
            pltpu.VMEM((tokens, height), narrow),
            pltpu.VMEM((tokens, width), narrow),
            pltpu.VMEM((width, rank), narrow),
            pltpu.VMEM((rank, tokens), narrow),
            pltpu.SemaphoreType.DMA((8,)),
        ],
        compiler_params=pltpu.CompilerParams(vmem_limit_bytes=20 * MIB),
        cost_estimate=cost,
        name="partner_low",
    )(core, rows0, cols0, rows1, cols1, in_bases)
    from_partner = swapped(theirs)
    mine = pl.pallas_call(
        own_kernel,
        out_shape=pltpu.VMEM((rank, height), wide),
        in_specs=[in_smem] + [in_hbm] * 2 + [in_vmem] * 3,
        out_specs=in_vmem,
        scratch_shapes=[
            pltpu.VMEM((tokens - early, height), narrow),
            pltpu.VMEM((rank, tokens), narrow),
            pltpu.SemaphoreType.DMA,
        ],
        compiler_params=pltpu.CompilerParams(vmem_limit_bytes=14 * MIB),
        cost_estimate=cost,
        name="own_low",
    )(core, rows0, rows1, rows, cols, base)
    return mine, from_partner


def combine_kernel(mine, partner, out, tiles, sems, *, n_x, n_y):
    count = out.shape[0] // sems.shape[0]
    for z in range(sems.shape[0]):
        for x in range(n_x):
            for y in range(n_y):
                ranks, rows = (pl.ds(x * LANES, LANES), pl.ds((z * n_y + y) * LANES, LANES))
                total = mine[ranks, rows] + partner[ranks, rows].astype(wide)
                tiles[(z * n_x + x) * n_y + y] = total.astype(narrow)
        at = pl.ds(z * count, count)
        pltpu.make_async_copy(tiles.at[at], out.at[at], sems.at[z]).start()
    for z in range(sems.shape[0]):
        at = pl.ds(z * count, count)
        pltpu.make_async_copy(tiles.at[at], out.at[at], sems.at[z]).wait()


def combine(mine, partner, n_z, n_y, n_x):
    shape = (n_z * n_y * n_x, LANES, LANES)
    return pl.pallas_call(
        functools.partial(combine_kernel, n_x=n_x, n_y=n_y),
        out_shape=pltpu.HBM(shape, narrow),
        in_specs=[in_vmem] * 2,
        out_specs=in_hbm,
        scratch_shapes=[pltpu.VMEM(shape, narrow), pltpu.SemaphoreType.DMA((n_z,))],
        compiler_params=pltpu.CompilerParams(vmem_limit_bytes=8 * MIB),
        name="combine",
    )(mine, partner)


def moments_kernel(core, low, firsts, seconds, got, first, second, direction):
    zero = core[0] == 0

    def joined(old, came):
        kept = jnp.where(zero, old[0], old[1])
        return jnp.concatenate((jnp.where(zero, kept, came), jnp.where(zero, came, kept)), axis=0)

    sums = low[...]
    first_new = first_decay * joined(firsts, got[0]) + (1.0 - first_decay) * sums
    second_new = second_decay * joined(seconds, got[1]) + (1.0 - second_decay) * sums * sums
    first[...] = first_new
    second[...] = second_new
    direction[...] = first_new / jnp.sqrt(second_new)


def new_moments(core, low, firsts, seconds, got):
    return pl.pallas_call(
        moments_kernel,
        out_shape=(pltpu.VMEM(low.shape, wide),) * 3,
        in_specs=[in_smem] + [in_vmem] * 4,
        out_specs=(in_vmem,) * 3,
        compiler_params=pltpu.CompilerParams(vmem_limit_bytes=4 * MIB),
        name="moments",
    )(core, low, firsts, seconds, got)


def fetch_kernel(where, bases, base, sem):
    cols = base.shape[0]
    at = pl.ds(pl.multiple_of(where[1] * cols, cols), cols)
    load = pltpu.make_async_copy(bases.at[where[0], at], base, sem)
    load.start()
    load.wait()


def own_base(where, bases, cols):
    return pl.pallas_call(
        fetch_kernel,
        out_shape=pltpu.VMEM((cols, bases.shape[2]), narrow),
        in_specs=[in_smem, in_hbm],
        out_specs=in_vmem,
        scratch_shapes=[pltpu.SemaphoreType.DMA],
        compiler_params=pltpu.CompilerParams(vmem_limit_bytes=2 * MIB),
        name="own_base",
    )(where, pltpu.with_memory_space_constraint(bases, pltpu.HBM))


def squares_kernel(*refs):
    *directions, row = refs
    total = jnp.zeros((1, LANES), wide)
    for part in directions:
        value = part[...]
        total = total + jnp.sum(value * value, axis=0, keepdims=True)
    row[...] = jnp.broadcast_to(jnp.sum(total, axis=1, keepdims=True), row.shape)


def squares_of(directions):
    return pl.pallas_call(
        squares_kernel,
        out_shape=pltpu.VMEM((8, LANES), wide),
        in_specs=[in_vmem] * len(directions),
        out_specs=in_vmem,
        compiler_params=pltpu.CompilerParams(vmem_limit_bytes=2 * MIB),
        name="squares",
    )(*directions)


def project_kernel(where, base, *refs):
    *directions, own, other = refs
    core, chip_x = (where[0], where[1])
    cols = own.shape[0]
    n_x = len(directions)
    total = jnp.zeros((2 * cols, own.shape[1]), wide)
    for x in range(n_x):
        part = directions[0][...]
        back = lax.rem(chip_x - x + n_x, n_x)
        for s in range(1, n_x):
            part = jnp.where(back == s, directions[s][...], part)
        width, n = part.shape
        high = part.astype(narrow)
        rest = part - high.astype(wide)
        middle = rest.astype(narrow)
        low = (rest - middle.astype(wide)).astype(narrow)
        limbs = jnp.concatenate((high, middle, low), axis=1)
        product = jnp.dot(
            base[:, x * width : (x + 1) * width], limbs, preferred_element_type=wide
        )
        total = total + (product[:, :n] + (product[:, n : 2 * n] + product[:, 2 * n :]))
    left, right = (total[:cols], total[cols:])
    own[...] = jnp.where(core == 0, left, right)
    other[...] = jnp.where(core == 0, right, left)


def project(where, base, directions, cols):
    out = pltpu.VMEM((cols, directions[0].shape[1]), wide)
    return pl.pallas_call(
        project_kernel,
        out_shape=(out, out),
        in_specs=[in_smem] + [in_vmem] * (1 + len(directions)),
        out_specs=(in_vmem,) * 2,
        compiler_params=pltpu.CompilerParams(vmem_limit_bytes=6 * MIB),
        name="project",
    )(where, base, *directions)


def from_others(array, axis):
    n = lax.axis_size(axis)
    return [
        lax.ppermute(array, axis, [(i, (i + s) % n) for i in range(n)]) for s in range(1, n)
    ]


def summed(array, axis):
    return functools.reduce(jnp.add, from_others(array, axis), array)


def steps_of(core, squares, partner_squares, own, came, key_weight, out_weight):
    def scale_of(total):
        return lax.rsqrt(total[0:1, 0:1] / (D * RANK) + 1.0)

    zero = core[0] == 0
    here, there = (own[...] * scale_of(squares), came[...] * scale_of(partner_squares))
    key_step = jnp.where(zero, here, there).T
    out_step = jnp.where(zero, there, here)
    key_new = key_weight[...] - learn_rate * key_step
    out_new = out_weight[...] - learn_rate * out_step
    return (key_new, out_new, key_step, out_step)


def copies_kernel(*refs):
    *ins, copies = refs
    key_new, out_new, _, _ = steps_of(*ins)
    copies[...] = jnp.broadcast_to(
        jnp.stack((key_new.astype(narrow), out_new.astype(narrow)))[None], copies.shape
    )


def steps_kernel(*refs):
    for out, value in zip(refs[-4:], steps_of(*refs[:-4])):
        out[...] = value


def stepped(kernel, outs, *args):
    return pl.pallas_call(
        kernel,
        out_shape=outs,
        in_specs=[in_smem] + [in_vmem] * 6,
        out_specs=jax.tree.map(lambda _: in_vmem, outs),
        compiler_params=pltpu.CompilerParams(vmem_limit_bytes=6 * MIB),
    )(*args)


def spread_kernel(gathered, key_copy, out_copy, *, n_y):
    n_z = gathered.shape[0] // n_y
    for y in range(n_y):
        for z in range(n_z):
            at = pl.ds((z * n_y + y) * LANES, LANES)
            key_copy[at, :] = gathered[y * n_z + z, 0]
            out_copy[:, at] = gathered[y * n_z + z, 1]


def spread(gathered, n_y):
    n_fs, _, rows, cols = gathered.shape
    return pl.pallas_call(
        functools.partial(spread_kernel, n_y=n_y),
        out_shape=(
            jax.ShapeDtypeStruct((n_fs * rows, cols), narrow),
            jax.ShapeDtypeStruct((cols, n_fs * rows), narrow),
        ),
        in_specs=[in_vmem],
        out_specs=(in_vmem, in_vmem),
        compiler_params=pltpu.CompilerParams(vmem_limit_bytes=6 * MIB),
        name="spread",
    )(gathered)


def body(
    saved_input,
    key_cot,
    mixed_out,
    out_cot,
    key_weight,
    out_weight,
    bases,
    first_moment,
    second_moment,
):
    core = lax.axis_index("tp_1").astype(jnp.int32)
    chip_x = lax.axis_index("tp_0").astype(jnp.int32)
    n_z, n_y, n_x = (lax.axis_size(axis) for axis in ("fs_0", "fs_1", "tp_0"))
    rows, cols = key_weight.shape
    half = first_moment.shape[2]
    this = core.reshape(1)

    mine, from_partner = both_low(this, saved_input, key_cot, out_cot, mixed_out, bases)
    arrived = exchanged(combine(mine, from_partner, n_z, n_y, n_x), CHIPS)
    low = arrived.astype(wide).sum(axis=0)

    firsts = first_moment.transpose(0, 2, 1)
    seconds = second_moment.transpose(0, 2, 1)
    got = swapped(
        jnp.stack((pick(core, firsts[1], firsts[0]), pick(core, seconds[1], seconds[0])))
    )
    first, second, direction = new_moments(this, low, firsts, seconds, got)

    where = jnp.stack((core, chip_x))
    base = own_base(where, bases, 2 * cols)
    directions = [direction] + from_others(direction, "tp_0")
    squares = summed(squares_of(directions), "fs_0")
    own, other = project(where, base, directions, cols)
    squares = summed(squares, "fs_1")
    came = swapped(other)
    partner_squares = swapped(squares)
    square = jax.ShapeDtypeStruct((rows, cols), wide)
    args = (this, squares, partner_squares, own, came, key_weight, out_weight)
    copies = stepped(copies_kernel, pltpu.HBM((n_z * n_y, 2, rows, cols), narrow), *args)
    gathered = exchanged(copies, ("fs_1", "fs_0"))
    key_new, out_new, key_step, out_step = stepped(steps_kernel, (square,) * 4, *args)
    key_copy, out_copy = spread(gathered, n_y)

    news = jnp.stack((first, second))
    low_half, high_half = (news[:, :half], news[:, half:])
    stay = pick(core, low_half, high_half)
    come = swapped(pick(core, high_half, low_half))
    key_moments = pick(core, stay, come)
    out_moments = pick(core, come, stay)
    first_new = jnp.stack((key_moments[0], out_moments[0])).transpose(0, 2, 1)
    second_new = jnp.stack((key_moments[1], out_moments[1])).transpose(0, 2, 1)
    return (key_new, out_new, key_step, out_step, first_new, second_new, key_copy, out_copy)


def solution(mesh):
    torus = Mesh(mesh.devices.reshape(4, 4, 4, 2), ("fs_0", "fs_1", "tp_0", "tp_1"))
    placed = (
        P(FS_TP, None),
        P(FS_TP, None),
        P(FS_TP, None),
        P(FS_TP, None),
        P(FS, TP),
        P(TP, FS),
        P(),
        P(None, FS, TP),
        P(None, FS, TP),
    )
    return jax.shard_map(
        body,
        mesh=torus,
        in_specs=placed,
        out_specs=(
            P(FS, TP),
            P(TP, FS),
            P(FS, TP),
            P(TP, FS),
            P(None, FS, TP),
            P(None, FS, TP),
            P(None, TP),
            P(TP, None),
        ),
        check_vma=False,
    )
```

```python
import functools

import jax
import jax.numpy as jnp
from jax import lax
from jax.experimental import pallas as pl
from jax.experimental.pallas import tpu as pltpu
from jax.sharding import Mesh
from jax.sharding import PartitionSpec as P

D = 2048
RANK = 512
FS = ("fs_0", "fs_1")
TP = ("tp_0", "tp_1")
CHIPS = ("fs_0", "tp_0", "fs_1")
FS_TP = ("fs_0", "fs_1", "tp_0", "tp_1")
SWAP = [(0, 1), (1, 0)]
LANES = 128
CHIPS_TURN = 42
SQUARES_TURN = 0
GATHER_TURN = 10
MIB = 2**20


first_decay = 0.8
second_decay = 0.9
learn_rate = 0.01

wide = jnp.float32
narrow = jnp.bfloat16
in_smem = pl.BlockSpec(memory_space=pltpu.SMEM)
in_hbm = pl.BlockSpec(memory_space=pltpu.HBM)
in_vmem = pl.BlockSpec(memory_space=pltpu.VMEM)


def turned(n, turn):
    return [(i + turn) % n for i in range(n)]


def exchanged(tiles, axes, turn=0):
    groups = [turned(lax.axis_size(axes), turn)] if turn else None
    return lax.all_to_all(
        tiles, axes, split_axis=0, concat_axis=0, axis_index_groups=groups, tiled=True
    )


def swapped(array):
    return lax.ppermute(array, "tp_1", SWAP)


def pick(core, zero, one):
    return jnp.where(core == 0, zero, one)


PARTS = 3
CHUNKS = 8


def map_part(i, cols, base, mapped):
    part = cols.shape[0] // PARTS
    at = pl.ds(i * part, part)
    block = jnp.dot(cols[at, :], base[...], preferred_element_type=wide)
    mapped[:, at] = block.astype(narrow).T


def contract(mapped, rows, out):
    chunk = out.shape[1] // CHUNKS
    for j in range(CHUNKS):
        at = pl.ds(j * chunk, chunk)
        total, start = (None, 0)
        for piece in rows:
            length = piece.shape[0]
            block = jnp.dot(
                mapped[:, start : start + length], piece[:, at], preferred_element_type=wide
            )
            total = block if total is None else total + block
            start += length
        out[:, at] = total.astype(out.dtype)


def partner_kernel(
    core, rows0, cols0, rows1, cols1, bases, out, rows2, cols2, base2, rows, cols, base, mapped, sems
):
    part = cols.shape[0] // PARTS
    early = rows2.shape[0]

    def base_load(k):
        matrix = core[0] if k else 1 - core[0]
        return pltpu.make_async_copy(bases.at[matrix], (base, base2)[k], sems.at[k])

    def cols_load(source, i):
        at = pl.ds(i * part, part)
        return pltpu.make_async_copy(source.at[at], cols.at[at], sems.at[2 + i])

    def rows_load(source):
        return pltpu.make_async_copy(source, rows, sems.at[5])

    def own_cols_load(source):
        return pltpu.make_async_copy(source, cols2, sems.at[6])

    def own_rows_load(source):
        return pltpu.make_async_copy(source.at[pl.ds(0, early)], rows2, sems.at[7])

    def start(zero, load, first, second):
        @pl.when(core[0] == zero)
        def _():
            load(first).start()

        @pl.when(core[0] != zero)
        def _():
            load(second).start()

    base_load(0).start()
    for i in range(PARTS):
        start(1, lambda source, i=i: cols_load(source, i), cols0, cols1)
    base_load(0).wait()
    for i in range(PARTS):
        cols_load(cols0, i).wait()
        if i == 0:
            start(1, rows_load, rows0, rows1)
        map_part(i, cols, base, mapped)
    rows_load(rows0).wait()
    base_load(1).start()
    start(0, own_cols_load, cols0, cols1)
    start(0, own_rows_load, rows0, rows1)
    contract(mapped, (rows,), out)
    base_load(1).wait()
    own_cols_load(cols0).wait()
    own_rows_load(rows0).wait()


def own_kernel(core, rows0, rows1, rows, cols, base, out, late, mapped, sem):
    def late_load(source):
        return pltpu.make_async_copy(source.at[pl.ds(rows.shape[0], late.shape[0])], late, sem)

    @pl.when(core[0] == 0)
    def _():
        late_load(rows0).start()

    @pl.when(core[0] != 0)
    def _():
        late_load(rows1).start()

    for i in range(PARTS):
        map_part(i, cols, base, mapped)
    late_load(rows0).wait()
    contract(mapped, (rows, late), out)


def cost_of(tokens, height, width, rank):
    return pl.CostEstimate(
        flops=2 * tokens * rank * (height + width),
        bytes_accessed=2 * tokens * (height + width),
        transcendentals=0,
    )


def both_low(core, saved_input, key_cot, out_cot, mixed_out, bases):
    tokens, height = saved_input.shape
    _, width, rank = bases.shape
    early = tokens // 2
    cost = cost_of(tokens, height, width, rank)
    rows0, cols0, rows1, cols1, in_bases = (
        pltpu.with_memory_space_constraint(a, pltpu.HBM)
        for a in (saved_input, key_cot, out_cot, mixed_out, bases)
    )
    theirs, rows, cols, base = pl.pallas_call(
        partner_kernel,
        out_shape=(
            pltpu.VMEM((rank, height), narrow),
            pltpu.VMEM((early, height), narrow),
            pltpu.VMEM((tokens, width), narrow),
            pltpu.VMEM((width, rank), narrow),
        ),
        in_specs=[in_smem] + [in_hbm] * 5,
        out_specs=(in_vmem,) * 4,
        scratch_shapes=[
            pltpu.VMEM((tokens, height), narrow),
            pltpu.VMEM((tokens, width), narrow),
            pltpu.VMEM((width, rank), narrow),
            pltpu.VMEM((rank, tokens), narrow),
            pltpu.SemaphoreType.DMA((8,)),
        ],
        compiler_params=pltpu.CompilerParams(vmem_limit_bytes=20 * MIB),
        cost_estimate=cost,
        name="partner_low",
    )(core, rows0, cols0, rows1, cols1, in_bases)
    from_partner = swapped(theirs)
    mine = pl.pallas_call(
        own_kernel,
        out_shape=pltpu.VMEM((rank, height), wide),
        in_specs=[in_smem] + [in_hbm] * 2 + [in_vmem] * 3,
        out_specs=in_vmem,
        scratch_shapes=[
            pltpu.VMEM((tokens - early, height), narrow),
            pltpu.VMEM((rank, tokens), narrow),
            pltpu.SemaphoreType.DMA,
        ],
        compiler_params=pltpu.CompilerParams(vmem_limit_bytes=14 * MIB),
        cost_estimate=cost,
        name="own_low",
    )(core, rows0, rows1, rows, cols, base)
    return mine, from_partner


def combine_kernel(mine, partner, out, tiles, sems, *, n_x, n_y):
    count = out.shape[0] // sems.shape[0]
    for j, chip in enumerate(turned(out.shape[0], CHIPS_TURN)):
        z, x, y = (chip // (n_x * n_y), chip // n_y % n_x, chip % n_y)
        ranks, rows = (pl.ds(x * LANES, LANES), pl.ds((z * n_y + y) * LANES, LANES))
        total = mine[ranks, rows] + partner[ranks, rows].astype(wide)
        tiles[j] = total.astype(narrow)
        if (j + 1) % count == 0:
            at = pl.ds(j + 1 - count, count)
            pltpu.make_async_copy(tiles.at[at], out.at[at], sems.at[j // count]).start()
    for k in range(sems.shape[0]):
        at = pl.ds(k * count, count)
        pltpu.make_async_copy(tiles.at[at], out.at[at], sems.at[k]).wait()


def combine(mine, partner, n_z, n_y, n_x):
    shape = (n_z * n_y * n_x, LANES, LANES)
    return pl.pallas_call(
        functools.partial(combine_kernel, n_x=n_x, n_y=n_y),
        out_shape=pltpu.HBM(shape, narrow),
        in_specs=[in_vmem] * 2,
        out_specs=in_hbm,
        scratch_shapes=[pltpu.VMEM(shape, narrow), pltpu.SemaphoreType.DMA((4,))],
        compiler_params=pltpu.CompilerParams(vmem_limit_bytes=8 * MIB),
        name="combine",
    )(mine, partner)


def moments_kernel(core, low, firsts, seconds, got, first, second, direction, row):
    zero = core[0] == 0

    def joined(old, came):
        kept = jnp.where(zero, old[0], old[1])
        return jnp.concatenate((jnp.where(zero, kept, came), jnp.where(zero, came, kept)), axis=0)

    sums = low[...]
    first_new = first_decay * joined(firsts, got[0]) + (1.0 - first_decay) * sums
    second_new = second_decay * joined(seconds, got[1]) + (1.0 - second_decay) * sums * sums
    ratio = first_new / jnp.sqrt(second_new)
    first[...] = first_new
    second[...] = second_new
    direction[...] = ratio
    square = jnp.sum(jnp.sum(ratio * ratio, axis=0, keepdims=True), axis=1, keepdims=True)
    lanes = lax.broadcasted_iota(jnp.int32, (1, LANES), 1)
    row[...] = jnp.broadcast_to(jnp.where(lanes == core[0], square, 0.0)[None], row.shape)


def new_moments(core, low, firsts, seconds, got, everyone):
    return pl.pallas_call(
        moments_kernel,
        out_shape=(pltpu.VMEM(low.shape, wide),) * 3
        + (pltpu.HBM((everyone, 1, LANES), wide),),
        in_specs=[in_smem] + [in_vmem] * 4,
        out_specs=(in_vmem,) * 4,
        compiler_params=pltpu.CompilerParams(vmem_limit_bytes=4 * MIB),
        name="moments",
    )(core, low, firsts, seconds, got)


def fetch_kernel(where, bases, base, sem):
    cols = base.shape[0]
    at = pl.ds(pl.multiple_of(where[1] * cols, cols), cols)
    load = pltpu.make_async_copy(bases.at[where[0], at], base, sem)
    load.start()
    load.wait()


def own_base(where, bases, cols):
    return pl.pallas_call(
        fetch_kernel,
        out_shape=pltpu.VMEM((cols, bases.shape[2]), narrow),
        in_specs=[in_smem, in_hbm],
        out_specs=in_vmem,
        scratch_shapes=[pltpu.SemaphoreType.DMA],
        compiler_params=pltpu.CompilerParams(vmem_limit_bytes=2 * MIB),
        name="own_base",
    )(where, pltpu.with_memory_space_constraint(bases, pltpu.HBM))


def project_kernel(where, base, *refs):
    *directions, own, other = refs
    core, chip_x = (where[0], where[1])
    cols = own.shape[0]
    n_x = len(directions)
    total = jnp.zeros((2 * cols, own.shape[1]), wide)
    for x in range(n_x):
        part = directions[0][...]
        back = lax.rem(chip_x - x + n_x, n_x)
        for s in range(1, n_x):
            part = jnp.where(back == s, directions[s][...], part)
        width, n = part.shape
        high = part.astype(narrow)
        rest = part - high.astype(wide)
        middle = rest.astype(narrow)
        low = (rest - middle.astype(wide)).astype(narrow)
        limbs = jnp.concatenate((high, middle, low), axis=1)
        product = jnp.dot(
            base[:, x * width : (x + 1) * width], limbs, preferred_element_type=wide
        )
        total = total + (product[:, :n] + (product[:, n : 2 * n] + product[:, 2 * n :]))
    left, right = (total[:cols], total[cols:])
    own[...] = jnp.where(core == 0, left, right)
    other[...] = jnp.where(core == 0, right, left)


def project(where, base, directions, cols):
    out = pltpu.VMEM((cols, directions[0].shape[1]), wide)
    return pl.pallas_call(
        project_kernel,
        out_shape=(out, out),
        in_specs=[in_smem] + [in_vmem] * (1 + len(directions)),
        out_specs=(in_vmem,) * 2,
        compiler_params=pltpu.CompilerParams(vmem_limit_bytes=6 * MIB),
        name="project",
    )(where, base, *directions)


def from_others(array, axis):
    n = lax.axis_size(axis)
    return [
        lax.ppermute(array, axis, [(i, (i + s) % n) for i in range(n)]) for s in range(1, n)
    ]


def steps_of(core, sums, own, came, key_weight, out_weight):
    scales = lax.rsqrt(jnp.sum(sums[...], axis=0) / (D * RANK) + 1.0)
    zero = core[0] == 0
    key_step = jnp.where(zero, own[...], came[...]).T * scales[:, 0:1]
    out_step = jnp.where(zero, came[...], own[...]) * scales[:, 1:2]
    key_new = key_weight[...] - learn_rate * key_step
    out_new = out_weight[...] - learn_rate * out_step
    return (key_new, out_new, key_step, out_step)


def copies_kernel(*refs):
    *ins, copies = refs
    key_new, out_new, _, _ = steps_of(*ins)
    copies[...] = jnp.broadcast_to(
        jnp.stack((key_new.astype(narrow), out_new.astype(narrow)))[None], copies.shape
    )


def steps_kernel(*refs):
    for out, value in zip(refs[-4:], steps_of(*refs[:-4])):
        out[...] = value


def stepped(kernel, outs, *args):
    return pl.pallas_call(
        kernel,
        out_shape=outs,
        in_specs=[in_smem] + [in_vmem] * 5,
        out_specs=jax.tree.map(lambda _: in_vmem, outs),
        compiler_params=pltpu.CompilerParams(vmem_limit_bytes=6 * MIB),
    )(*args)


def spread_kernel(gathered, key_copy, out_copy, *, n_y):
    n_z = gathered.shape[0] // n_y
    for i, source in enumerate(turned(gathered.shape[0], GATHER_TURN)):
        y, z = divmod(source, n_z)
        at = pl.ds((z * n_y + y) * LANES, LANES)
        key_copy[at, :] = gathered[i, 0]
        out_copy[:, at] = gathered[i, 1]


def spread(gathered, n_y):
    n_fs, _, rows, cols = gathered.shape
    return pl.pallas_call(
        functools.partial(spread_kernel, n_y=n_y),
        out_shape=(
            jax.ShapeDtypeStruct((n_fs * rows, cols), narrow),
            jax.ShapeDtypeStruct((cols, n_fs * rows), narrow),
        ),
        in_specs=[in_vmem],
        out_specs=(in_vmem, in_vmem),
        compiler_params=pltpu.CompilerParams(vmem_limit_bytes=6 * MIB),
        name="spread",
    )(gathered)


def body(
    saved_input,
    key_cot,
    mixed_out,
    out_cot,
    key_weight,
    out_weight,
    bases,
    first_moment,
    second_moment,
):
    core = lax.axis_index("tp_1").astype(jnp.int32)
    chip_x = lax.axis_index("tp_0").astype(jnp.int32)
    n_z, n_y, n_x = (lax.axis_size(axis) for axis in ("fs_0", "fs_1", "tp_0"))
    rows, cols = key_weight.shape
    half = first_moment.shape[2]
    this = core.reshape(1)

    mine, from_partner = both_low(this, saved_input, key_cot, out_cot, mixed_out, bases)
    arrived = exchanged(combine(mine, from_partner, n_z, n_y, n_x), CHIPS, CHIPS_TURN)
    low = arrived.astype(wide).sum(axis=0)

    firsts = first_moment.transpose(0, 2, 1)
    seconds = second_moment.transpose(0, 2, 1)
    got = swapped(
        jnp.stack((pick(core, firsts[1], firsts[0]), pick(core, seconds[1], seconds[0])))
    )
    first, second, direction, row = new_moments(
        this, low, firsts, seconds, got, lax.axis_size(FS_TP)
    )

    where = jnp.stack((core, chip_x))
    base = own_base(where, bases, 2 * cols)
    directions = [direction] + from_others(direction, "tp_0")
    sums = exchanged(row, FS_TP, SQUARES_TURN)
    own, other = project(where, base, directions, cols)
    came = swapped(other)
    square = jax.ShapeDtypeStruct((rows, cols), wide)
    args = (this, sums, own, came, key_weight, out_weight)
    copies = stepped(copies_kernel, pltpu.HBM((n_z * n_y, 2, rows, cols), narrow), *args)
    gathered = exchanged(copies, ("fs_1", "fs_0"), GATHER_TURN)
    key_new, out_new, key_step, out_step = stepped(steps_kernel, (square,) * 4, *args)
    key_copy, out_copy = spread(gathered, n_y)

    news = jnp.stack((first, second))
    low_half, high_half = (news[:, :half], news[:, half:])
    stay = pick(core, low_half, high_half)
    come = swapped(pick(core, high_half, low_half))
    key_moments = pick(core, stay, come)
    out_moments = pick(core, come, stay)
    first_new = jnp.stack((key_moments[0], out_moments[0])).transpose(0, 2, 1)
    second_new = jnp.stack((key_moments[1], out_moments[1])).transpose(0, 2, 1)
    return (key_new, out_new, key_step, out_step, first_new, second_new, key_copy, out_copy)


def solution(mesh):
    torus = Mesh(mesh.devices.reshape(4, 4, 4, 2), ("fs_0", "fs_1", "tp_0", "tp_1"))
    placed = (
        P(FS_TP, None),
        P(FS_TP, None),
        P(FS_TP, None),
        P(FS_TP, None),
        P(FS, TP),
        P(TP, FS),
        P(),
        P(None, FS, TP),
        P(None, FS, TP),
    )
    return jax.shard_map(
        body,
        mesh=torus,
        in_specs=placed,
        out_specs=(
            P(FS, TP),
            P(TP, FS),
            P(FS, TP),
            P(TP, FS),
            P(None, FS, TP),
            P(None, FS, TP),
            P(None, TP),
            P(TP, None),
        ),
        check_vma=False,
    )
```

```python
import functools

import jax
import jax.numpy as jnp
from jax import lax
from jax.experimental import pallas as pl
from jax.experimental.pallas import tpu as pltpu
from jax.sharding import Mesh
from jax.sharding import PartitionSpec as P

D = 2048
RANK = 512
FS = ("fs_0", "fs_1")
TP = ("tp_0", "tp_1")
CHIPS = ("fs_0", "tp_0", "fs_1")
FS_TP = ("fs_0", "fs_1", "tp_0", "tp_1")
SWAP = [(0, 1), (1, 0)]
LANES = 128
CHIPS_TURN = 43
SQUARES_TURN = 0
GATHER_TURN = 14
MIB = 2**20


first_decay = 0.8
second_decay = 0.9
learn_rate = 0.01

wide = jnp.float32
narrow = jnp.bfloat16
in_smem = pl.BlockSpec(memory_space=pltpu.SMEM)
in_hbm = pl.BlockSpec(memory_space=pltpu.HBM)
in_vmem = pl.BlockSpec(memory_space=pltpu.VMEM)


def turned(n, turn):
    return [(i + turn) % n for i in range(n)]


def exchanged(tiles, axes, turn=0):
    groups = [turned(lax.axis_size(axes), turn)] if turn else None
    return lax.all_to_all(
        tiles, axes, split_axis=0, concat_axis=0, axis_index_groups=groups, tiled=True
    )


def swapped(array):
    return lax.ppermute(array, "tp_1", SWAP)


def pick(core, zero, one):
    return jnp.where(core == 0, zero, one)


PARTS = 3
CHUNKS = 8


def map_part(i, cols, base, mapped):
    part = cols.shape[0] // PARTS
    at = pl.ds(i * part, part)
    block = jnp.dot(cols[at, :], base[...], preferred_element_type=wide)
    mapped[:, at] = block.astype(narrow).T


def contract(mapped, rows, out):
    chunk = out.shape[1] // CHUNKS
    for j in range(CHUNKS):
        at = pl.ds(j * chunk, chunk)
        total, start = (None, 0)
        for piece in rows:
            length = piece.shape[0]
            block = jnp.dot(
                mapped[:, start : start + length], piece[:, at], preferred_element_type=wide
            )
            total = block if total is None else total + block
            start += length
        out[:, at] = total.astype(out.dtype)


def partner_kernel(
    core, rows0, cols0, rows1, cols1, bases, out, rows2, cols2, base2, rows, cols, base, mapped, sems
):
    part = cols.shape[0] // PARTS
    early = rows2.shape[0]

    def base_load(k):
        matrix = core[0] if k else 1 - core[0]
        return pltpu.make_async_copy(bases.at[matrix], (base, base2)[k], sems.at[k])

    def cols_load(source, i):
        at = pl.ds(i * part, part)
        return pltpu.make_async_copy(source.at[at], cols.at[at], sems.at[2 + i])

    def rows_load(source):
        return pltpu.make_async_copy(source, rows, sems.at[5])

    def own_cols_load(source):
        return pltpu.make_async_copy(source, cols2, sems.at[6])

    def own_rows_load(source):
        return pltpu.make_async_copy(source.at[pl.ds(0, early)], rows2, sems.at[7])

    def start(zero, load, first, second):
        @pl.when(core[0] == zero)
        def _():
            load(first).start()

        @pl.when(core[0] != zero)
        def _():
            load(second).start()

    base_load(0).start()
    for i in range(PARTS):
        start(1, lambda source, i=i: cols_load(source, i), cols0, cols1)
    base_load(0).wait()
    for i in range(PARTS):
        cols_load(cols0, i).wait()
        if i == 0:
            start(1, rows_load, rows0, rows1)
        map_part(i, cols, base, mapped)
    rows_load(rows0).wait()
    base_load(1).start()
    start(0, own_cols_load, cols0, cols1)
    start(0, own_rows_load, rows0, rows1)
    contract(mapped, (rows,), out)
    base_load(1).wait()
    own_cols_load(cols0).wait()
    own_rows_load(rows0).wait()


def own_kernel(core, rows0, rows1, rows, cols, base, out, late, mapped, sem):
    def late_load(source):
        return pltpu.make_async_copy(source.at[pl.ds(rows.shape[0], late.shape[0])], late, sem)

    @pl.when(core[0] == 0)
    def _():
        late_load(rows0).start()

    @pl.when(core[0] != 0)
    def _():
        late_load(rows1).start()

    for i in range(PARTS):
        map_part(i, cols, base, mapped)
    late_load(rows0).wait()
    contract(mapped, (rows, late), out)


def cost_of(tokens, height, width, rank):
    return pl.CostEstimate(
        flops=2 * tokens * rank * (height + width),
        bytes_accessed=2 * tokens * (height + width),
        transcendentals=0,
    )


def both_low(core, saved_input, key_cot, out_cot, mixed_out, bases):
    tokens, height = saved_input.shape
    _, width, rank = bases.shape
    early = 2 * tokens // 3
    cost = cost_of(tokens, height, width, rank)
    rows0, cols0, rows1, cols1, in_bases = (
        pltpu.with_memory_space_constraint(a, pltpu.HBM)
        for a in (saved_input, key_cot, out_cot, mixed_out, bases)
    )
    theirs, rows, cols, base = pl.pallas_call(
        partner_kernel,
        out_shape=(
            pltpu.VMEM((rank, height), narrow),
            pltpu.VMEM((early, height), narrow),
            pltpu.VMEM((tokens, width), narrow),
            pltpu.VMEM((width, rank), narrow),
        ),
        in_specs=[in_smem] + [in_hbm] * 5,
        out_specs=(in_vmem,) * 4,
        scratch_shapes=[
            pltpu.VMEM((tokens, height), narrow),
            pltpu.VMEM((tokens, width), narrow),
            pltpu.VMEM((width, rank), narrow),
            pltpu.VMEM((rank, tokens), narrow),
            pltpu.SemaphoreType.DMA((8,)),
        ],
        compiler_params=pltpu.CompilerParams(vmem_limit_bytes=20 * MIB),
        cost_estimate=cost,
        name="partner_low",
    )(core, rows0, cols0, rows1, cols1, in_bases)
    from_partner = swapped(theirs)
    mine = pl.pallas_call(
        own_kernel,
        out_shape=pltpu.VMEM((rank, height), wide),
        in_specs=[in_smem] + [in_hbm] * 2 + [in_vmem] * 3,
        out_specs=in_vmem,
        scratch_shapes=[
            pltpu.VMEM((tokens - early, height), narrow),
            pltpu.VMEM((rank, tokens), narrow),
            pltpu.SemaphoreType.DMA,
        ],
        compiler_params=pltpu.CompilerParams(vmem_limit_bytes=14 * MIB),
        cost_estimate=cost,
        name="own_low",
    )(core, rows0, rows1, rows, cols, base)
    return mine, from_partner


def combine_kernel(mine, partner, out, tiles, sems, *, n_x, n_y):
    count = out.shape[0] // sems.shape[0]
    for j, chip in enumerate(turned(out.shape[0], CHIPS_TURN)):
        z, x, y = (chip // (n_x * n_y), chip // n_y % n_x, chip % n_y)
        ranks, rows = (pl.ds(x * LANES, LANES), pl.ds((z * n_y + y) * LANES, LANES))
        total = mine[ranks, rows] + partner[ranks, rows].astype(wide)
        tiles[j] = total.astype(narrow)
        if (j + 1) % count == 0:
            at = pl.ds(j + 1 - count, count)
            pltpu.make_async_copy(tiles.at[at], out.at[at], sems.at[j // count]).start()
    for k in range(sems.shape[0]):
        at = pl.ds(k * count, count)
        pltpu.make_async_copy(tiles.at[at], out.at[at], sems.at[k]).wait()


def combine(mine, partner, n_z, n_y, n_x):
    shape = (n_z * n_y * n_x, LANES, LANES)
    return pl.pallas_call(
        functools.partial(combine_kernel, n_x=n_x, n_y=n_y),
        out_shape=pltpu.HBM(shape, narrow),
        in_specs=[in_vmem] * 2,
        out_specs=in_hbm,
        scratch_shapes=[pltpu.VMEM(shape, narrow), pltpu.SemaphoreType.DMA((4,))],
        compiler_params=pltpu.CompilerParams(vmem_limit_bytes=8 * MIB),
        name="combine",
    )(mine, partner)


def moments_kernel(core, low, firsts, seconds, got, first, second, direction, row):
    zero = core[0] == 0

    def joined(old, came):
        kept = jnp.where(zero, old[0], old[1])
        return jnp.concatenate((jnp.where(zero, kept, came), jnp.where(zero, came, kept)), axis=0)

    sums = low[...]
    first_new = first_decay * joined(firsts, got[0]) + (1.0 - first_decay) * sums
    second_new = second_decay * joined(seconds, got[1]) + (1.0 - second_decay) * sums * sums
    ratio = first_new / jnp.sqrt(second_new)
    first[...] = first_new
    second[...] = second_new
    direction[...] = ratio
    square = jnp.sum(jnp.sum(ratio * ratio, axis=0, keepdims=True), axis=1, keepdims=True)
    lanes = lax.broadcasted_iota(jnp.int32, (1, LANES), 1)
    row[...] = jnp.broadcast_to(jnp.where(lanes == core[0], square, 0.0)[None], row.shape)


def new_moments(core, low, firsts, seconds, got, everyone):
    return pl.pallas_call(
        moments_kernel,
        out_shape=(pltpu.VMEM(low.shape, wide),) * 3
        + (pltpu.VMEM((everyone, 1, LANES), wide),),
        in_specs=[in_smem] + [in_vmem] * 4,
        out_specs=(in_vmem,) * 4,
        compiler_params=pltpu.CompilerParams(vmem_limit_bytes=4 * MIB),
        name="moments",
    )(core, low, firsts, seconds, got)


def fetch_kernel(where, bases, base, sem):
    cols = base.shape[0]
    at = pl.ds(pl.multiple_of(where[1] * cols, cols), cols)
    load = pltpu.make_async_copy(bases.at[where[0], at], base, sem)
    load.start()
    load.wait()


def own_base(where, bases, cols):
    return pl.pallas_call(
        fetch_kernel,
        out_shape=pltpu.VMEM((cols, bases.shape[2]), narrow),
        in_specs=[in_smem, in_hbm],
        out_specs=in_vmem,
        scratch_shapes=[pltpu.SemaphoreType.DMA],
        compiler_params=pltpu.CompilerParams(vmem_limit_bytes=2 * MIB),
        name="own_base",
    )(where, pltpu.with_memory_space_constraint(bases, pltpu.HBM))


def project_kernel(where, base, *refs):
    *directions, own, other = refs
    core, chip_x = (where[0], where[1])
    cols = own.shape[0]
    n_x = len(directions)
    total = jnp.zeros((2 * cols, own.shape[1]), wide)
    for x in range(n_x):
        part = directions[0][...]
        back = lax.rem(chip_x - x + n_x, n_x)
        for s in range(1, n_x):
            part = jnp.where(back == s, directions[s][...], part)
        width, n = part.shape
        high = part.astype(narrow)
        rest = part - high.astype(wide)
        middle = rest.astype(narrow)
        low = (rest - middle.astype(wide)).astype(narrow)
        limbs = jnp.concatenate((high, middle, low), axis=1)
        product = jnp.dot(
            base[:, x * width : (x + 1) * width], limbs, preferred_element_type=wide
        )
        total = total + (product[:, :n] + (product[:, n : 2 * n] + product[:, 2 * n :]))
    left, right = (total[:cols], total[cols:])
    own[...] = jnp.where(core == 0, left, right)
    other[...] = jnp.where(core == 0, right, left)


def project(where, base, directions, cols):
    out = pltpu.VMEM((cols, directions[0].shape[1]), wide)
    return pl.pallas_call(
        project_kernel,
        out_shape=(out, out),
        in_specs=[in_smem] + [in_vmem] * (1 + len(directions)),
        out_specs=(in_vmem,) * 2,
        compiler_params=pltpu.CompilerParams(vmem_limit_bytes=6 * MIB),
        name="project",
    )(where, base, *directions)


def from_others(array, axis):
    n = lax.axis_size(axis)
    return [
        lax.ppermute(array, axis, [(i, (i + s) % n) for i in range(n)]) for s in range(1, n)
    ]


def steps_of(core, sums, own, came, key_weight, out_weight):
    scales = lax.rsqrt(jnp.sum(sums[...], axis=0) / (D * RANK) + 1.0)
    zero = core[0] == 0
    key_step = jnp.where(zero, own[...], came[...]).T * scales[:, 0:1]
    out_step = jnp.where(zero, came[...], own[...]) * scales[:, 1:2]
    key_new = key_weight[...] - learn_rate * key_step
    out_new = out_weight[...] - learn_rate * out_step
    return (key_new, out_new, key_step, out_step)


def copies_kernel(*refs):
    *ins, copies = refs
    key_new, out_new, _, _ = steps_of(*ins)
    copies[...] = jnp.broadcast_to(
        jnp.stack((key_new.astype(narrow), out_new.astype(narrow)))[None], copies.shape
    )


def steps_kernel(*refs):
    for out, value in zip(refs[-4:], steps_of(*refs[:-4])):
        out[...] = value


def stepped(kernel, outs, *args):
    return pl.pallas_call(
        kernel,
        out_shape=outs,
        in_specs=[in_smem] + [in_vmem] * 5,
        out_specs=jax.tree.map(lambda _: in_vmem, outs),
        compiler_params=pltpu.CompilerParams(vmem_limit_bytes=6 * MIB),
    )(*args)


def spread_kernel(gathered, key_copy, out_copy, *, n_y):
    n_z = gathered.shape[0] // n_y
    for i, source in enumerate(turned(gathered.shape[0], GATHER_TURN)):
        y, z = divmod(source, n_z)
        at = pl.ds((z * n_y + y) * LANES, LANES)
        key_copy[at, :] = gathered[i, 0]
        out_copy[:, at] = gathered[i, 1]


def spread(gathered, n_y):
    n_fs, _, rows, cols = gathered.shape
    return pl.pallas_call(
        functools.partial(spread_kernel, n_y=n_y),
        out_shape=(
            jax.ShapeDtypeStruct((n_fs * rows, cols), narrow),
            jax.ShapeDtypeStruct((cols, n_fs * rows), narrow),
        ),
        in_specs=[in_vmem],
        out_specs=(in_vmem, in_vmem),
        compiler_params=pltpu.CompilerParams(vmem_limit_bytes=6 * MIB),
        name="spread",
    )(gathered)


def body(
    saved_input,
    key_cot,
    mixed_out,
    out_cot,
    key_weight,
    out_weight,
    bases,
    first_moment,
    second_moment,
):
    core = lax.axis_index("tp_1").astype(jnp.int32)
    chip_x = lax.axis_index("tp_0").astype(jnp.int32)
    n_z, n_y, n_x = (lax.axis_size(axis) for axis in ("fs_0", "fs_1", "tp_0"))
    rows, cols = key_weight.shape
    half = first_moment.shape[2]
    this = core.reshape(1)

    mine, from_partner = both_low(this, saved_input, key_cot, out_cot, mixed_out, bases)
    arrived = exchanged(combine(mine, from_partner, n_z, n_y, n_x), CHIPS, CHIPS_TURN)
    low = arrived.astype(wide).sum(axis=0)

    firsts = first_moment.transpose(0, 2, 1)
    seconds = second_moment.transpose(0, 2, 1)
    got = swapped(
        jnp.stack((pick(core, firsts[1], firsts[0]), pick(core, seconds[1], seconds[0])))
    )
    first, second, direction, row = new_moments(
        this, low, firsts, seconds, got, lax.axis_size(FS_TP)
    )

    where = jnp.stack((core, chip_x))
    base = own_base(where, bases, 2 * cols)
    directions = [direction] + from_others(direction, "tp_0")
    sums = exchanged(row, FS_TP, SQUARES_TURN)
    own, other = project(where, base, directions, cols)
    came = swapped(other)
    square = jax.ShapeDtypeStruct((rows, cols), wide)
    args = (this, sums, own, came, key_weight, out_weight)
    copies = stepped(copies_kernel, pltpu.HBM((n_z * n_y, 2, rows, cols), narrow), *args)
    gathered = exchanged(copies, ("fs_1", "fs_0"), GATHER_TURN)
    key_new, out_new, key_step, out_step = stepped(steps_kernel, (square,) * 4, *args)
    key_copy, out_copy = spread(gathered, n_y)

    news = jnp.stack((first, second))
    low_half, high_half = (news[:, :half], news[:, half:])
    stay = pick(core, low_half, high_half)
    come = swapped(pick(core, high_half, low_half))
    key_moments = pick(core, stay, come)
    out_moments = pick(core, come, stay)
    first_new = jnp.stack((key_moments[0], out_moments[0])).transpose(0, 2, 1)
    second_new = jnp.stack((key_moments[1], out_moments[1])).transpose(0, 2, 1)
    return (key_new, out_new, key_step, out_step, first_new, second_new, key_copy, out_copy)


def solution(mesh):
    torus = Mesh(mesh.devices.reshape(4, 4, 4, 2), ("fs_0", "fs_1", "tp_0", "tp_1"))
    placed = (
        P(FS_TP, None),
        P(FS_TP, None),
        P(FS_TP, None),
        P(FS_TP, None),
        P(FS, TP),
        P(TP, FS),
        P(),
        P(None, FS, TP),
        P(None, FS, TP),
    )
    return jax.shard_map(
        body,
        mesh=torus,
        in_specs=placed,
        out_specs=(
            P(FS, TP),
            P(TP, FS),
            P(FS, TP),
            P(TP, FS),
            P(None, FS, TP),
            P(None, FS, TP),
            P(None, TP),
            P(TP, None),
        ),
        check_vma=False,
    )
```
